256 devices in a mesh: sp: 64 (over z, y, core), tp: 4 (over x).
Axes of the slice: x: 4, y: 4, z: 8, core: 2. Of those that a mesh axis runs over, the one named last changes fastest.
Arguments:
- residual: bfloat16 [24576, 2048], P(('sp', 'tp')), may hold values from -6 to 6
- query_one: bfloat16 [24576, 512], P('sp', 'tp'), may hold values from -6 to 6
- key_one: bfloat16 [24576, 512], P('sp', 'tp'), may hold values from -6 to 6
- value_one: bfloat16 [24576, 1024], P('sp', 'tp'), may hold values from -6 to 6
- gate_one: bfloat16 [24576, 1024], P('sp', 'tp'), may hold values from -6 to 6
- decay_one: bfloat16 [2, 24576, 512], P(None, 'sp', 'tp'), may hold values from -12 to 12
- norm_one: float32 [128], replicated, may hold values from 0.1 to 1.9
- output_one: bfloat16 [1024, 2048], P('tp'), may hold values from -0.125 to 0.125
- query_two: bfloat16 [24576, 1024], P('sp', 'tp'), may hold values from -6 to 6
- key_two: bfloat16 [24576, 1024], P('sp', 'tp'), may hold values from -6 to 6
- value_two: bfloat16 [24576, 1024], P('sp', 'tp'), may hold values from -6 to 6
- gate_two: bfloat16 [24576, 1024], P('sp', 'tp'), may hold values from -6 to 6
- decay_two: bfloat16 [2, 24576, 1024], P(None, 'sp', 'tp'), may hold values from -12 to 12
- norm_two: float32 [128], replicated, may hold values from 0.1 to 1.9
- output_two: bfloat16 [1024, 2048], P('tp'), may hold values from -0.125 to 0.125
- norm_gain: float32 [2048], replicated, may hold values from 0.1 to 1.9
- expert_ids: int32 [24576, 2], P('sp'), may hold values from 0 to 63, as said below
- group_weight: float32 [24576], P('sp'), may hold values from 0.25 to 1
- pair_weight: float32 [24576, 2], P('sp'), may hold values from 0.05 to 1
- expert_gate: bfloat16 [64, 2048, 1024], P('sp', None, 'tp'), may hold values from -0.125 to 0.125
- expert_up: bfloat16 [64, 2048, 1024], P('sp', None, 'tp'), may hold values from -0.125 to 0.125
- expert_down: bfloat16 [64, 1024, 2048], P('sp', 'tp'), may hold values from -0.1875 to 0.1875
Outputs:
- layer_out: bfloat16 [24576, 2048], P(('sp', 'tp'))
The draws below stay inside these ranges and needn't reach their ends.
Inputs may be any that keep to these rules, and one draw needn't show every extreme that they name: `expert_ids`: each row names two different experts of one group, the group of expert e being e // 16. In each aligned block of 96 rows no expert is named more than 4 times, and one expert, the same in every block, is named exactly 4 times in each block.
All inputs are finite; a program needn't handle non-finite values.
Results may differ from the reference program's by a relative error of at most 0.018.
Values may be sent and summed in bfloat16 or wider, within the bound.
No kernel may reach another device: no remote copies, remote signals or barrier semaphores. Data moves between devices by JAX's collectives and lax.ppermute only.
A program may use at most 128 MiB of HBM per device.

```python
import math
from functools import partial
import jax
import jax.numpy as jnp
from jax import lax

D = 2048
HEADS_ONE = 8
KEY_ONE = 64
HEADS_TWO = 8
KEY_TWO = 128
VALUE_W = 128
FF = 1024
BLOCK = 64
GROUPS = 4
TOK_DEV = 384
SEQUENCE_TOKENS = 24576
ROWS_DEV = 96
EXPERTS = 64
EXP_GROUP = 16
CAPACITY = 4
N_TP = 4


def decay_law(key, channels):
    random_keys = jax.random.split(key, 6)
    slow = jax.random.uniform(random_keys[0], (2, 1, channels)) < 0.5
    random_jitter = 0.5 * jax.random.normal(random_keys[1], (2, SEQUENCE_TOKENS, channels))
    channel_factor = jnp.exp(jax.random.uniform(random_keys[2], (2, 1, channels), minval=math.log(0.5), maxval=math.log(1.5)))
    device_factor = jnp.exp(jax.random.uniform(random_keys[3], (2, SEQUENCE_TOKENS // TOK_DEV, 1), minval=math.log(0.5), maxval=math.log(1.5)))
    device_factor = jnp.repeat(device_factor, TOK_DEV, axis=1)
    slow_rate = 0.35 * channel_factor * device_factor / SEQUENCE_TOKENS
    fast_rate = 1.0 / (BLOCK * channel_factor)
    rate = jnp.where(slow, slow_rate, fast_rate)
    smoothed_values = -jnp.log(jnp.expm1(16.0 * rate)) + random_jitter
    spike_position = jax.random.randint(random_keys[4], (2, 2, 1), 0, SEQUENCE_TOKENS)
    retained_entries = jax.random.uniform(random_keys[5], (2, 2, 1), minval=0.5, maxval=0.8)
    spike_value = -jnp.log(jnp.expm1(-16.0 * jnp.log(retained_entries)))
    token_positions = jnp.arange(SEQUENCE_TOKENS, dtype=jnp.int32)[None, None, :]
    match_flags = token_positions == spike_position
    spike_row = jnp.sum(jnp.where(match_flags, spike_value, 0.0), axis=1)
    any_match_found = jnp.any(match_flags, axis=1)
    final_output = jnp.where(any_match_found[:, :, None], spike_row[:, :, None] + 0.1 * random_jitter, smoothed_values)
    return jnp.clip(final_output, -12.0, 12.0).astype(jnp.bfloat16)


def draw_decay_one(key, part):
    return decay_law(jax.random.fold_in(key, 11), HEADS_ONE * KEY_ONE)


def draw_decay_two(key, part):
    return decay_law(jax.random.fold_in(key, 12), HEADS_TWO * KEY_TWO)


def route_block(key, hot):
    order_key, group_key, member_key = jax.random.split(key, 3)
    order = jax.random.permutation(order_key, ROWS_DEV).astype(jnp.int32)
    group_score = jax.random.randint(group_key, (ROWS_DEV, GROUPS), 0, 1 << 20) * GROUPS + jnp.arange(GROUPS, dtype=jnp.int32)
    member_score = jax.random.randint(member_key, (ROWS_DEV, EXPERTS), 0, 1 << 20) * EXPERTS + jnp.arange(EXPERTS, dtype=jnp.int32)
    labels = jnp.arange(EXPERTS, dtype=jnp.int32)

    def place_row(counts, step):
        row = order[step]
        forced = step < CAPACITY
        free = counts < CAPACITY
        usable = jnp.sum(free.reshape(GROUPS, EXP_GROUP).astype(jnp.int32), axis=1) >= 2
        picked_group = jnp.argmax(jnp.where(usable, group_score[row], -1)).astype(jnp.int32)
        chosen_group = jnp.where(forced, hot // EXP_GROUP, picked_group)
        allowed = free & (labels // EXP_GROUP == chosen_group)
        scored = jnp.where(allowed, member_score[row], -1)
        first = jnp.where(forced, hot, jnp.argmax(scored).astype(jnp.int32))
        second = jnp.argmax(jnp.where(labels == first, -1, scored)).astype(jnp.int32)
        counts = counts + (labels == first).astype(jnp.int32) + (labels == second).astype(jnp.int32)
        return (counts, (row, first, second))
    _, (rows, firsts, seconds) = lax.scan(place_row, jnp.zeros((EXPERTS,), jnp.int32), jnp.arange(ROWS_DEV, dtype=jnp.int32))
    return jnp.zeros((ROWS_DEV, 2), jnp.int32).at[rows].set(jnp.stack([firsts, seconds], axis=1))


def draw_expert_ids(key, part):
    hot_key, block_key = jax.random.split(jax.random.fold_in(key, 21))
    hot = jax.random.randint(hot_key, (), 0, EXPERTS).astype(jnp.int32)
    random_keys = jax.random.split(block_key, SEQUENCE_TOKENS // ROWS_DEV)
    blocks = jax.vmap(partial(route_block, hot=hot))(random_keys)
    return blocks.reshape(SEQUENCE_TOKENS, 2)


def levels(key, shape, shards, low, high):
    level = 1.0
    for axis_at, shards_of in shards:
        draws = jax.random.uniform(jax.random.fold_in(jax.random.fold_in(key, 6), axis_at), (shards_of,), jnp.float32, low / len(shards), high / len(shards))
        level = level * jnp.repeat(jnp.exp(draws), shape[axis_at] // shards_of).reshape((-1,) + (1,) * (len(shape) - 1 - axis_at))
    return level


def bell_draw(rng, shape, spread, most, shards=(), kind=jnp.bfloat16):
    values = spread * jax.random.normal(rng, shape, jnp.float32)
    if shards:
        values = values * levels(rng, shape, shards, -0.22, 0.18)
    return jnp.clip(values, -most, most).astype(kind)


def setup_inputs(seed: int = 0) -> dict:
    streams_of = jax.random.split(jax.random.key(seed), 23)
    return {
        "residual": bell_draw(streams_of[0], (SEQUENCE_TOKENS, D), 1.0, 6.0, ((0, 256),)),
        "query_one": bell_draw(streams_of[1], (SEQUENCE_TOKENS, HEADS_ONE * KEY_ONE), 1.0, 6.0, ((0, 64), (1, 4))),
        "key_one": bell_draw(streams_of[2], (SEQUENCE_TOKENS, HEADS_ONE * KEY_ONE), 1.0, 6.0, ((0, 64), (1, 4))),
        "value_one": bell_draw(streams_of[3], (SEQUENCE_TOKENS, HEADS_ONE * VALUE_W), 1.0, 6.0, ((0, 64), (1, 4))),
        "gate_one": bell_draw(streams_of[4], (SEQUENCE_TOKENS, HEADS_ONE * VALUE_W), 1.0, 6.0, ((0, 64), (1, 4))),
        "decay_one": draw_decay_one(jax.random.fold_in(streams_of[22], 71), 0),
        "norm_one": jnp.clip(1.0 + 0.18 * jax.random.normal(streams_of[6], (VALUE_W,), jnp.float32), 0.1, 1.9),
        "output_one": bell_draw(streams_of[7], (HEADS_ONE * VALUE_W, D), ((HEADS_ONE + HEADS_TWO) * VALUE_W) ** -0.5, 0.125, ((0, 4),)),
        "query_two": bell_draw(streams_of[8], (SEQUENCE_TOKENS, HEADS_TWO * KEY_TWO), 1.0, 6.0, ((0, 64), (1, 4))),
        "key_two": bell_draw(streams_of[9], (SEQUENCE_TOKENS, HEADS_TWO * KEY_TWO), 1.0, 6.0, ((0, 64), (1, 4))),
        "value_two": bell_draw(streams_of[10], (SEQUENCE_TOKENS, HEADS_TWO * VALUE_W), 1.0, 6.0, ((0, 64), (1, 4))),
        "gate_two": bell_draw(streams_of[11], (SEQUENCE_TOKENS, HEADS_TWO * VALUE_W), 1.0, 6.0, ((0, 64), (1, 4))),
        "decay_two": draw_decay_two(jax.random.fold_in(streams_of[22], 71), 0),
        "norm_two": jnp.clip(1.0 + 0.18 * jax.random.normal(streams_of[13], (VALUE_W,), jnp.float32), 0.1, 1.9),
        "output_two": bell_draw(streams_of[14], (HEADS_TWO * VALUE_W, D), ((HEADS_ONE + HEADS_TWO) * VALUE_W) ** -0.5, 0.125, ((0, 4),)),
        "norm_gain": jnp.clip(1.0 + 0.18 * jax.random.normal(streams_of[15], (D,), jnp.float32), 0.1, 1.9),
        "expert_ids": draw_expert_ids(jax.random.fold_in(streams_of[22], 71), 0),
        "group_weight": jnp.clip(jnp.exp(math.log(1.0) - 1.3862944 * jax.random.uniform(streams_of[17], (SEQUENCE_TOKENS,), jnp.float32) ** levels(streams_of[17], (SEQUENCE_TOKENS,), ((0, 64),), -0.2, 0.2)), 0.25, 1.0),
        "pair_weight": jnp.clip(jnp.exp(math.log(1.0) - 2.9957323 * jax.random.uniform(streams_of[18], (SEQUENCE_TOKENS, 2), jnp.float32) ** levels(streams_of[18], (SEQUENCE_TOKENS, 2), ((0, 64),), -0.2, 0.2)), 0.05, 1.0),
        "expert_gate": bell_draw(streams_of[19], (EXPERTS, D, FF), D ** -0.5, 0.125, ((0, 64), (2, 4))),
        "expert_up": bell_draw(streams_of[20], (EXPERTS, D, FF), D ** -0.5, 0.125, ((0, 64), (2, 4))),
        "expert_down": bell_draw(streams_of[21], (EXPERTS, FF, D), FF ** -0.5, 0.1875, ((0, 64), (1, 4))),
    }


HIGH = lax.Precision.HIGHEST
TAU = 16.0
EPS = 1e-06

def advance(state_now, step_input):
    fade_rate, extra_term = step_input
    return (fade_rate[..., None] * state_now + extra_term, state_now)

def block_pass(queries, key_rows, values, rates):
    length, heads, width = queries.shape
    blocks = length // BLOCK
    shaped = (blocks, BLOCK, heads, width)
    cumul = jnp.cumsum(rates.reshape(shaped), axis=1)
    block_end = cumul[:, -1]
    key_blocks = key_rows.reshape(shaped)
    value_blocks = values.reshape(blocks, BLOCK, heads, values.shape[-1])
    query_dec = queries.reshape(shaped) * jnp.exp(cumul)
    query_low = query_dec.astype(jnp.bfloat16)
    key_dec = (key_blocks * jnp.exp(-cumul)).astype(jnp.bfloat16)
    key_end = (key_blocks * jnp.exp(block_end[:, None] - cumul)).astype(jnp.bfloat16)
    lower_mask = jnp.tril(jnp.ones((BLOCK, BLOCK), jnp.float32))
    scores = jnp.einsum('nthd,nshd->nhts', query_low, key_dec, preferred_element_type=jnp.float32) * lower_mask
    scores = scores.astype(jnp.bfloat16)
    inner_part = jnp.einsum('nhts,nshe->nthe', scores, value_blocks, preferred_element_type=jnp.float32)
    added = jnp.einsum('nshd,nshe->nhde', key_end, value_blocks, preferred_element_type=jnp.float32)
    empty = jnp.zeros((heads, width, values.shape[-1]), jnp.float32)
    state_out, before = lax.scan(advance, empty, (jnp.exp(block_end), added))
    outer_part = jnp.einsum('nthd,nhde->nthe', query_dec, before, precision=HIGH)
    return (inner_part + outer_part).reshape(length, heads, values.shape[-1])

def group_mix(query, key_in, value, gate, decay, gain, width):
    heads = query.shape[1] // width
    queries = query.astype(jnp.float32).reshape(SEQUENCE_TOKENS, heads, width) * width ** (-0.5)
    key_rows = key_in.astype(jnp.float32).reshape(SEQUENCE_TOKENS, heads, width)
    values = value.reshape(SEQUENCE_TOKENS, heads, VALUE_W)
    rates = jax.nn.log_sigmoid(decay.astype(jnp.float32)) / TAU
    ahead = block_pass(queries, key_rows, values, rates[0].reshape(SEQUENCE_TOKENS, heads, width))
    behind = block_pass(jnp.flip(queries, 0), jnp.flip(key_rows, 0), jnp.flip(values, 0), jnp.flip(rates[1], 0).reshape(SEQUENCE_TOKENS, heads, width))
    total = ahead + jnp.flip(behind, 0)
    scale = lax.rsqrt(lax.optimization_barrier(jnp.mean(total * total, axis=-1, keepdims=True)) + EPS)
    normed = (total * scale * gain).reshape(SEQUENCE_TOKENS, heads * VALUE_W)
    return (normed * jax.nn.silu(gate.astype(jnp.float32))).astype(jnp.bfloat16)

def rounded(term):
    return lax.optimization_barrier(term.astype(jnp.bfloat16)).astype(jnp.float32)

def slot_table(routes, capacity, experts):
    flat = routes.reshape(-1)
    count = flat.shape[0]
    onehot = (flat[:, None] == jnp.arange(experts, dtype=jnp.int32)[None, :]).astype(jnp.int32)
    place = lax.optimization_barrier(jnp.sum((jnp.cumsum(onehot, axis=0) - onehot) * onehot, axis=1)).astype(jnp.int32)
    table = jnp.full((experts, capacity), count, jnp.int32).at[flat, place].set(jnp.arange(count, dtype=jnp.int32))
    return (table, place)

def reference(residual, query_one, key_one, value_one, gate_one, decay_one, norm_one, output_one, query_two, key_two, value_two, gate_two, decay_two, norm_two, output_two, norm_gain, expert_ids, group_weight, pair_weight, expert_gate, expert_up, expert_down):
    mixed_one = group_mix(query_one, key_one, value_one, gate_one, decay_one, norm_one, KEY_ONE)
    mixed_two = group_mix(query_two, key_two, value_two, gate_two, decay_two, norm_two, KEY_TWO)
    span_one = mixed_one.shape[1] // N_TP
    span_two = mixed_two.shape[1] // N_TP
    projected = jnp.zeros((SEQUENCE_TOKENS, D), jnp.float32)
    for part in range(N_TP):
        term = jnp.dot(mixed_one[:, part * span_one:(part + 1) * span_one], output_one[part * span_one:(part + 1) * span_one], preferred_element_type=jnp.float32)
        term = term + jnp.dot(mixed_two[:, part * span_two:(part + 1) * span_two], output_two[part * span_two:(part + 1) * span_two], preferred_element_type=jnp.float32)
        projected = projected + rounded(term)
    stream = (residual.astype(jnp.float32) + rounded(projected)).astype(jnp.bfloat16)
    wide = stream.astype(jnp.float32)
    normed = (wide * lax.rsqrt(lax.optimization_barrier(jnp.mean(wide * wide, axis=-1, keepdims=True)) + EPS) * norm_gain).astype(jnp.bfloat16)
    weights = group_weight[:, None] * pair_weight / lax.optimization_barrier(jnp.sum(pair_weight, axis=1, keepdims=True))
    blocks = SEQUENCE_TOKENS // ROWS_DEV
    tables, places = jax.vmap(partial(slot_table, capacity=CAPACITY, experts=EXPERTS))(expert_ids.reshape(blocks, ROWS_DEV, 2))
    offsets = (jnp.arange(blocks, dtype=jnp.int32) * (2 * ROWS_DEV))[:, None, None]
    assigned = jnp.where(tables == 2 * ROWS_DEV, 2 * SEQUENCE_TOKENS, tables + offsets).astype(jnp.int32)
    assigned = jnp.transpose(assigned, (1, 0, 2)).reshape(EXPERTS, blocks * CAPACITY)
    padded = jnp.concatenate([normed, jnp.zeros((1, D), jnp.bfloat16)], axis=0)
    route_weight = jnp.concatenate([weights.reshape(-1), jnp.zeros((1,), jnp.float32)])
    span = FF // N_TP

    def expert_pass(total, step_input):
        index, weight_gate, weight_up, weight_down = step_input
        token = index // 2
        rows = padded[token]
        gate_part = jnp.dot(rows, weight_gate, preferred_element_type=jnp.float32)
        up_part = jnp.dot(rows, weight_up, preferred_element_type=jnp.float32)
        hidden = (jax.nn.silu(gate_part) * up_part).astype(jnp.bfloat16)
        summed = jnp.zeros((rows.shape[0], D), jnp.float32)
        for part in range(N_TP):
            summed = summed + rounded(jnp.dot(hidden[:, part * span:(part + 1) * span], weight_down[part * span:(part + 1) * span], preferred_element_type=jnp.float32))
        final_output = rounded(summed)
        return (total.at[token].add(route_weight[index][:, None] * final_output), None)
    total, _ = lax.scan(expert_pass, jnp.zeros((SEQUENCE_TOKENS + 1, D), jnp.float32), (assigned, expert_gate, expert_up, expert_down))
    return (stream.astype(jnp.float32) + total[:SEQUENCE_TOKENS]).astype(jnp.bfloat16)
```

```python
import jax
import jax.numpy as jnp
from jax import lax
from jax.experimental import pallas as pl
from jax.experimental.pallas import tpu as pltpu
from jax.sharding import Mesh
from jax.sharding import PartitionSpec as P

D = 2048
T = 384
ROWS = 96
BLOCK = 64
NBLK = T // BLOCK
KEYS = 384
PEERS = 64
OWN = 12
PAD = 16
HALF = PEERS // 2 * PAD
EXPERTS = 64
CAP = 4
SLOTS = EXPERTS * CAP
FFS = 256
SP = ("sp_0", "sp_1", "sp_2")
SP_TP = ("sp_0", "sp_1", "sp_2", "tp")
F32 = jnp.float32
BF = jnp.bfloat16
EPS = 1e-06


def iota(shape, dim):
    return lax.broadcasted_iota(jnp.int32, shape, dim)


def dot(a, b, dims=((1,), (0,))):
    return lax.dot_general(a, b, (dims, ((), ())), preferred_element_type=F32)


def split(x):
    hi = x.astype(BF)
    return hi, (x - hi.astype(F32)).astype(BF)


def log_rate(x):
    x = x.astype(F32)
    return (jnp.minimum(x, 0.0) - jnp.log1p(jnp.exp(-jnp.abs(x)))) * (1.0 / 16.0)


def rates_of(d1, d2, way):
    return jnp.concatenate([log_rate(d1[way]), log_rate(d2[way])], axis=1)


def tri_sum(mask, rate):
    ones = jnp.where(mask, 1.0, 0.0).astype(BF)
    hi, lo = split(rate)
    return dot(ones, hi) + dot(ones, lo)


def spread_matrix():
    row, key = iota((HALF, KEYS), 0), iota((HALF, KEYS), 1)
    return (row % PAD < OWN) & (row // PAD * OWN + row % PAD == key)


def states_body(k1, k2, v1, v2, d1, d2, out):
    keys = jnp.concatenate([k1[...].astype(F32), k2[...].astype(F32)], axis=1)
    row, col = iota((T, T), 0), iota((T, T), 1)
    spread = jnp.where(spread_matrix(), 1.0, 0.0).astype(BF)
    prow, pkey = iota((HALF, KEYS), 0), iota((HALF, KEYS), 1)
    mine = prow // PAD == pkey // OWN
    lanes = jnp.where(iota((KEYS, 128), 0) % OWN == iota((KEYS, 128), 1), 1.0, 0.0)
    lanes = lanes.astype(BF)
    for way in range(2):
        rate = rates_of(d1, d2, way)
        rest = tri_sum(col > row if way == 0 else col < row, rate)
        faded = (keys * jnp.exp(rest)).astype(BF)
        pair = dot(faded[:, :128], v1[...], ((0,), (0,)))
        upper = iota((128, 128), 0) < 64
        parts = [jnp.where(upper, pair[:, :128], pair[:, 128:])]
        for h in range(2):
            parts.append(
                dot(
                    faded[:, 128 + 128 * h : 256 + 128 * h],
                    v2[:, 128 * h : 128 * h + 128],
                    ((0,), (0,)),
                )
            )
        state = jnp.concatenate(parts, axis=0).astype(BF)
        hi, lo = split(jnp.sum(rate, axis=0, keepdims=True))
        hi, lo = hi.astype(F32), lo.astype(F32)
        tagged = jnp.where(prow % PAD == OWN, hi, jnp.where(prow % PAD == OWN + 1, lo, 0.0))
        tagged = jnp.where(mine, tagged, 0.0).astype(BF)
        out[HALF * way : HALF * way + HALF, :] = (
            dot(spread, state) + dot(tagged, lanes)
        ).astype(BF)


def scan_body(place, got, out, fade):
    pick = iota((PEERS, PAD, 128), 1) == iota((PEERS, PAD, 128), 2)
    rows = got[...].astype(F32)
    total = rows[:, OWN : OWN + 1, :] + rows[:, OWN + 1 : OWN + 2, :]
    log = jnp.sum(jnp.where(pick, total, 0.0), axis=2, keepdims=True)
    fade[...] = jnp.broadcast_to(jnp.exp(log), (PEERS, PAD, 128))
    forward = place[0] < PEERS // 2
    valid = iota((PAD, 128), 0) < OWN

    def step(k, carry):
        at = jnp.where(forward, k, PEERS - 1 - k)
        out[at] = jnp.where(valid, carry, 0.0).astype(BF)
        return carry * fade[at] + got[at].astype(F32)

    lax.fori_loop(0, PEERS, step, jnp.zeros((PAD, 128), F32), unroll=4)


def local_body(q1, q2, k1, k2, v1, v2, d1, d2, out, reach, st, sq, sk, sr):
    queries = jnp.concatenate(
        [q1[...].astype(F32) * 0.125, q2[...].astype(F32) * (128**-0.5)], axis=1
    )
    keys = jnp.concatenate([k1[...].astype(F32), k2[...].astype(F32)], axis=1)
    row, col = iota((T, T), 0), iota((T, T), 1)
    same = row // BLOCK == col // BLOCK
    gather = (iota((KEYS, HALF), 1) % PAD < OWN) & (
        iota((KEYS, HALF), 1) // PAD * OWN + iota((KEYS, HALF), 1) % PAD == iota((KEYS, HALF), 0)
    )
    gather = jnp.where(gather, 1.0, 0.0).astype(BF)
    ends = []
    for way in range(2):
        rate = rates_of(d1, d2, way)
        within = tri_sum(same & ((col <= row) if way == 0 else (col >= row)), rate)
        ahead = tri_sum((col <= row) if way == 0 else (col >= row), rate)
        rest = tri_sum(same & ((col > row) if way == 0 else (col < row)), rate)
        sq[way] = (queries * jnp.exp(within)).astype(BF)
        sk[way] = (keys * jnp.exp(-within)).astype(BF)
        sr[way] = (keys * jnp.exp(rest)).astype(BF)
        far = (queries * jnp.exp(ahead)).astype(BF)
        reach[:, HALF * way : HALF * way + HALF] = dot(far, gather).astype(BF)
        edge = BLOCK - 1 if way == 0 else 0
        ends.append(
            [jnp.exp(within[BLOCK * n + edge : BLOCK * n + edge + 1, :]) for n in range(NBLK)]
        )
    lane = iota((BLOCK, 128), 1)
    lower = iota((BLOCK, BLOCK), 1) <= iota((BLOCK, BLOCK), 0)
    higher = iota((BLOCK, BLOCK), 1) >= iota((BLOCK, BLOCK), 0)

    def owned(x, h):
        if h > 1:
            return x
        return jnp.where((lane < 64) if h == 0 else (lane >= 64), x, jnp.zeros_like(x))

    def value(h, n):
        ref, at = (v1, h) if h < 2 else (v2, h - 2)
        return ref[BLOCK * n : BLOCK * n + BLOCK, 128 * at : 128 * at + 128]

    for h in range(4):
        base = 0 if h < 2 else 128 * (h - 1)
        for way in range(2):
            state = jnp.zeros((128, 128), F32)
            order = range(NBLK) if way == 0 else reversed(range(NBLK))
            for n in order:
                st[h, n, :, 128 * way : 128 * way + 128] = state.astype(BF)
                kr = owned(sr[way, BLOCK * n : BLOCK * n + BLOCK, base : base + 128], h)
                state = state * ends[way][n][:, base : base + 128] + dot(
                    value(h, n), kr, ((0,), (0,))
                )
        for n in range(NBLK):
            at = slice(BLOCK * n, BLOCK * n + BLOCK)
            qf = owned(sq[0, at, base : base + 128], h)
            qb = owned(sq[1, at, base : base + 128], h)
            kf = sk[0, at, base : base + 128]
            kb = sk[1, at, base : base + 128]
            one = jnp.where(lower, dot(qf, kf, ((1,), (1,))), 0.0)
            two = jnp.where(higher, dot(qb, kb, ((1,), (1,))), 0.0)
            both = (one.astype(BF).astype(F32) + two.astype(BF).astype(F32)).astype(BF)
            res = dot(both, value(h, n))
            res = res + dot(jnp.concatenate([qf, qb], axis=1), st[h, n], ((1,), (1,)))
            out[at, 128 * h : 128 * h + 128] = res


RANGES = ((0, 64, 0, 128), (64, 128, 0, 256), (128, 256, 128, 384), (256, 384, 256, 512))


def finish_body(carried, reach, local, g1, g2, n1, n2, w1, w2, out, mixed):
    for h in range(4):
        first, last, low, high = RANGES[h]
        lane = iota((T, high - low), 1) + low
        key = lane // PAD * OWN + lane % PAD
        mask = (lane % PAD < OWN) & (key >= first) & (key < last)
        total = local[:, 128 * h : 128 * h + 128]
        for way in range(2):
            at = slice(HALF * way + low, HALF * way + high)
            q = jnp.where(mask, reach[:, at], jnp.zeros((T, high - low), BF))
            total = total + dot(q, carried[at, :])
        scale = lax.rsqrt(jnp.mean(total * total, axis=1, keepdims=True) + EPS)
        gate, gain = (g1, n1) if h < 2 else (g2, n2)
        u = gate[:, 128 * (h % 2) : 128 * (h % 2) + 128].astype(F32)
        silu = u / (1.0 + jnp.exp(-u))
        mixed[:, 128 * h : 128 * h + 128] = (total * scale * gain[...] * silu).astype(BF)
    for c in range(4):
        at = slice(512 * c, 512 * c + 512)
        out[:, at] = (
            dot(mixed[:, :256], w1[:, at]) + dot(mixed[:, 256:], w2[:, at])
        ).astype(BF)


def routes_body(rank, ids, group, pair, hot, high, low):
    at = pl.ds(rank[0] * ROWS, ROWS)
    own = ids[at, :]
    lane = iota((ROWS, EXPERTS), 1)
    named = [jnp.where(own[:, k : k + 1] == lane, 1.0, 0.0) for k in range(2)]
    before = jnp.where(iota((ROWS, ROWS), 1) < iota((ROWS, ROWS), 0), 1.0, 0.0).astype(BF)
    count = dot(before, (named[0] + named[1]).astype(BF))
    weight = pair[at, :]
    scaled = group[at, :] * weight / (weight[:, 0:1] + weight[:, 1:2])
    slot_lane = iota((ROWS, SLOTS), 1)
    marks = []
    for k in range(2):
        nth = jnp.sum(count * named[k], axis=1, keepdims=True).astype(jnp.int32)
        marks.append(own[:, k : k + 1] * CAP + nth == slot_lane)
    hot[...] = (jnp.where(marks[0], 1.0, 0.0) + jnp.where(marks[1], 1.0, 0.0)).astype(BF)
    spread = jnp.where(marks[0], scaled[:, 0:1], 0.0) + jnp.where(marks[1], scaled[:, 1:2], 0.0)
    hi, lo = split(spread)
    high[...] = hi
    low[...] = lo


def norm_body(parts, residual, gain, hot, stream, send):
    summed = parts[0].astype(F32)
    for p in range(1, 4):
        summed = summed + parts[p].astype(F32)
    wide = (residual[...].astype(F32) + summed.astype(BF).astype(F32)).astype(BF)
    stream[...] = wide
    wide = wide.astype(F32)
    scale = lax.rsqrt(jnp.mean(wide * wide, axis=1, keepdims=True) + EPS)
    normed = (wide * scale * gain[...]).astype(BF)
    send[...] = dot(hot[...], normed, ((0,), (0,))).astype(BF)


def expert_body(rows, *refs):
    weights, (out, wg, wu, wd, sems, acc) = refs[:12], refs[12:]
    copies = []
    for q in range(4):
        for k, buf in enumerate((wg, wu, wd)):
            copies.append(pltpu.make_async_copy(weights[3 * q + k], buf.at[q], sems.at[q, k]))
    for c in copies:
        c.start()
    x = rows[...]
    for q in range(4):
        copies[3 * q].wait()
        copies[3 * q + 1].wait()
        g = dot(x, wg[q])
        u = dot(x, wu[q])
        hidden = (g / (1.0 + jnp.exp(-g)) * u).astype(BF)
        copies[3 * q + 2].wait()
        for c in range(4):
            at = slice(512 * c, 512 * c + 512)
            part = dot(hidden, wd[q, :, at])
            if q == 0:
                acc[:, at] = part
            elif q < 3:
                acc[:, at] += part
            else:
                out[:, at] = (acc[:, at] + part).astype(BF)


def combine_body(stream, high, low, back, out):
    got = back[...]
    total = dot(high[...], got) + dot(low[...], got)
    out[...] = (stream[...].astype(F32) + total).astype(BF)


VMEM = pl.BlockSpec(memory_space=pltpu.VMEM)
SMEM = pl.BlockSpec(memory_space=pltpu.SMEM)
ANY = pl.BlockSpec(memory_space=pl.ANY)


def call(body, outs, *args, specs=None, scratch=(), flops=1000000):
    shapes = [jax.ShapeDtypeStruct(s, d) for s, d in outs]
    single = len(shapes) == 1
    return pl.pallas_call(
        body,
        out_shape=shapes[0] if single else shapes,
        in_specs=specs or [VMEM] * len(args),
        out_specs=VMEM if single else [VMEM] * len(shapes),
        scratch_shapes=list(scratch),
        compiler_params=pltpu.CompilerParams(vmem_limit_bytes=60 * 2**20),
        cost_estimate=pl.CostEstimate(flops=flops, transcendentals=0, bytes_accessed=4000000),
    )(*args)


def shifted(x, by):
    return lax.ppermute(x, "tp", [(i, (i + by) % 4) for i in range(4)])


def body(
    residual,
    query_one,
    key_one,
    value_one,
    gate_one,
    decay_one,
    norm_one,
    output_one,
    query_two,
    key_two,
    value_two,
    gate_two,
    decay_two,
    norm_two,
    output_two,
    norm_gain,
    expert_ids,
    group_weight,
    pair_weight,
    expert_gate,
    expert_up,
    expert_down,
):
    own = (expert_gate[0], expert_up[0], expert_down[0])
    left = [shifted(w, 1) for w in own]
    right = [shifted(w, 3) for w in own]
    payload = call(
        states_body,
        [((2 * HALF, 128), BF)],
        key_one,
        key_two,
        value_one,
        value_two,
        decay_one,
        decay_two,
        flops=10**9,
    )
    got = lax.all_to_all(payload.reshape(PEERS, PAD, 128), SP, 0, 0, tiled=True)
    place = lax.axis_index(SP).astype(jnp.int32).reshape(1)
    entering = call(
        scan_body,
        [((PEERS, PAD, 128), BF)],
        place,
        got,
        specs=[SMEM, VMEM],
        scratch=[pltpu.VMEM((PEERS, PAD, 128), F32)],
    )
    carried = lax.all_to_all(entering, SP, 0, 0, tiled=True).reshape(2 * HALF, 128)
    local, reach = call(
        local_body,
        [((T, 512), F32), ((T, 2 * HALF), BF)],
        query_one,
        query_two,
        key_one,
        key_two,
        value_one,
        value_two,
        decay_one,
        decay_two,
        scratch=[
            pltpu.VMEM((4, NBLK, 128, 256), BF),
            pltpu.VMEM((2, T, KEYS), BF),
            pltpu.VMEM((2, T, KEYS), BF),
            pltpu.VMEM((2, T, KEYS), BF),
        ],
        flops=10**10,
    )
    rank = lax.axis_index("tp").astype(jnp.int32).reshape(1)
    hot, high, low = call(
        routes_body,
        [((ROWS, SLOTS), BF)] * 3,
        rank,
        expert_ids,
        group_weight.reshape(T, 1),
        pair_weight,
        specs=[SMEM, VMEM, VMEM, VMEM],
    )
    head_part = call(
        finish_body,
        [((T, D), BF)],
        carried,
        reach,
        local,
        gate_one,
        gate_two,
        norm_one.reshape(1, 128),
        norm_two.reshape(1, 128),
        output_one,
        output_two,
        scratch=[pltpu.VMEM((T, 512), BF)],
        flops=10**9,
    )
    parts = lax.all_to_all(head_part.reshape(4, ROWS, D), "tp", 0, 0, tiled=True)
    (left, right), parts = lax.optimization_barrier(((left, right), parts))
    far = [
        shifted(left[0], 1),
        jnp.concatenate([shifted(left[1][:1024], 1), shifted(right[1][1024:], 3)], axis=0),
        shifted(right[2], 3),
    ]
    stream, send = call(
        norm_body,
        [((ROWS, D), BF), ((SLOTS, D), BF)],
        parts,
        residual,
        norm_gain.reshape(1, D),
        hot,
    )
    rows = lax.all_to_all(send.reshape(EXPERTS, CAP, D), SP, 0, 0, tiled=True)
    outs = call(
        expert_body,
        [((SLOTS, D), BF)],
        rows.reshape(SLOTS, D),
        *own,
        *left,
        *right,
        *far,
        specs=[VMEM] + [ANY] * 12,
        scratch=[
            pltpu.VMEM((4, D, FFS), BF),
            pltpu.VMEM((4, D, FFS), BF),
            pltpu.VMEM((4, FFS, D), BF),
            pltpu.SemaphoreType.DMA((4, 3)),
            pltpu.VMEM((SLOTS, D), F32),
        ],
        flops=3 * 10**9,
    )
    back = lax.all_to_all(outs.reshape(EXPERTS, CAP, D), SP, 0, 0, tiled=True)
    return call(combine_body, [((ROWS, D), BF)], stream, high, low, back.reshape(SLOTS, D))


def solution(mesh):
    torus = Mesh(mesh.devices.reshape(8, 4, 2, mesh.shape["tp"]), SP_TP)
    in_specs = (
        P(SP_TP, None),
        P(SP, "tp"),
        P(SP, "tp"),
        P(SP, "tp"),
        P(SP, "tp"),
        P(None, SP, "tp"),
        P(),
        P("tp", None),
        P(SP, "tp"),
        P(SP, "tp"),
        P(SP, "tp"),
        P(SP, "tp"),
        P(None, SP, "tp"),
        P(),
        P("tp", None),
        P(),
        P(SP, None),
        P(SP),
        P(SP, None),
        P(SP, None, "tp"),
        P(SP, None, "tp"),
        P(SP, "tp", None),
    )
    out_specs = P(SP_TP, None)
    return jax.shard_map(body, mesh=torus, in_specs=in_specs, out_specs=out_specs, check_vma=False)
```
